32 devices in a mesh: sp: 8 (over z, x), dp: 4 (over y, core).
Axes of the slice: x: 2, y: 2, z: 4, core: 2. Of those that a mesh axis runs over, the one named last changes fastest.
Arguments:
- gate_in: bfloat16 [4, 4096, 1024], P('dp', 'sp'), may hold values from -6 to 6
- value_in: bfloat16 [4, 4096, 1024], P('dp', 'sp'), may hold values from -6 to 6
- segments: int32 [4, 4096], P('dp', 'sp'), may hold values from 0 to 1, never falling along the last dimension, each value on 1 to 3072 neighbouring positions
- value_gain: bfloat16 [1024], P('sp'), may hold values from 0.099609375 to 1.8984375
- mixing: bfloat16 [8, 1024, 1024], P('sp', 'dp'), may hold values from -0.1875 to 0.1875
- mixing_bias: bfloat16 [8, 1024], P('sp'), may hold values from 0.099609375 to 1.8984375
Outputs:
- gated: bfloat16 [4, 4096, 1024], P('dp', 'sp')
The draws below stay inside these ranges and needn't reach their ends.
Inputs may be any that keep to these rules, and one draw needn't show every extreme that they name: `segments`: within each sequence the numbers never fall, every number 0 to 1 occurs, a document spans at most 3072 positions and some document spans exactly that.
All inputs are finite; a program needn't handle non-finite values.
Results may differ from the reference program's by a relative error of at most 0.0054.
Values may be sent and summed in bfloat16 or wider, within the bound.
No kernel may reach another device: no remote copies, remote signals or barrier semaphores. Data moves between devices by JAX's collectives and lax.ppermute only.
A program may use at most 128 MiB of HBM per device.

```python
import math
import jax
import jax.numpy as jnp
import numpy as np
from jax import lax

HEAD_DIM = 128
HEADS = 8
WIDTH = 1024
BLK = 1024
TOK_DEV = 512
SEQ = 4096
SEQS = 4
DOCS = 2


def steps_of(rng, dims, pieces, low, top_value):
    loudness, own = 1.0, jax.random.fold_in(rng, 6)
    for position, parts in pieces:
        heights = jnp.exp(jax.random.uniform(jax.random.fold_in(own, position), (parts,), jnp.float32, low / len(pieces), top_value / len(pieces)))
        loudness = loudness * jnp.repeat(heights, dims[position] // parts).reshape([-1 if axis == position else 1 for axis in range(len(dims))])
    return loudness


def split_up(count, total, reach, skew):
    portions = [(1 << 20) // math.isqrt(standing ** skew) + 1 for standing in range(2, count + 1)]
    spare, given = total - reach - (count - 1), [1] * (count - 1)
    while spare > 0:
        candidates = [i for i in range(count - 1) if given[i] < reach]
        whole, remaining = sum([portions[i] for i in candidates]), spare
        for i in candidates:
            extra = min(reach - given[i], max(1, remaining * portions[i] // whole), spare)
            given[i] = given[i] + extra
            spare = spare - extra
    return np.array([reach] + given)


def uneven(stream_key, number_of, total, bound, slope):
    if number_of == 2:
        one = jax.random.randint(stream_key, (), max(1, total - bound), min(bound, total - 1) + 1)
        return jnp.stack([one, total - one])
    sizes = jnp.asarray(split_up(number_of, total, bound, slope), jnp.int32)
    twos = (number_of - 1) // 2
    source_of, sink = sizes[1:1 + 2 * twos:2], sizes[2:2 + 2 * twos:2]
    margin = jnp.minimum(source_of - 1, bound - sink)
    shifted = jax.random.randint(jax.random.fold_in(stream_key, 1), (twos,), 0, 1 << 20) % (margin + 1)
    sizes = sizes.at[1:1 + 2 * twos:2].set(source_of - shifted).at[2:2 + 2 * twos:2].set(sink + shifted)
    return sizes[jax.random.permutation(jax.random.fold_in(stream_key, 2), number_of)]


def gaussian(key, shape, scale, limit, pieces=(), held_as=jnp.bfloat16):
    gain = steps_of(key, shape, pieces, -0.22, 0.18) if pieces else 1.0
    drawn = jax.random.normal(key, shape, jnp.float32) * scale * gain
    return jnp.minimum(jnp.maximum(drawn, -limit), limit).astype(held_as)


def setup_inputs(seed: int = 0) -> dict:
    seeds = jax.random.split(jax.random.key(seed), 7)
    gate_in = gaussian(seeds[0], (SEQS, SEQ, WIDTH), 1.0, 6.0, ((0, 4), (1, 8)))
    value_in = gaussian(seeds[1], (SEQS, SEQ, WIDTH), 1.0, 6.0, ((0, 4), (1, 8)))
    segments = jax.vmap(lambda own: jnp.searchsorted(jnp.cumsum(uneven(own, DOCS, SEQ, 6 * TOK_DEV, 0)), jnp.arange(SEQ), side="right"))(jax.random.split(seeds[2], SEQS)).reshape((SEQS, SEQ)).astype(jnp.int32)
    value_gain = jnp.clip(1.0 + 0.18 * jax.random.normal(seeds[3], (WIDTH,), jnp.float32), 0.099609375, 1.8984375).astype(jnp.bfloat16)
    mixing = gaussian(seeds[4], (HEADS, BLK, BLK), BLK ** -0.5, 0.1875, ((0, 8), (1, 4)))
    mixing_bias = jnp.clip(1.0 + 0.18 * jax.random.normal(seeds[5], (HEADS, BLK), jnp.float32), 0.099609375, 1.8984375).astype(jnp.bfloat16)
    return dict(gate_in=gate_in, value_in=value_in, segments=segments, value_gain=value_gain, mixing=mixing, mixing_bias=mixing_bias)


epsilon = 1e-06

def reference(gate_in, value_in, segments, value_gain, mixing, mixing_bias):
    seqs, length, width = value_in.shape
    values = jax.nn.gelu(value_in.astype(jnp.float32)).reshape(seqs, length, HEADS, HEAD_DIM)
    scaled = values * lax.rsqrt(lax.optimization_barrier(jnp.mean(values * values, axis=-1, keepdims=True)) + epsilon)
    normed = (scaled.reshape(seqs, length, width) * value_gain.astype(jnp.float32)).astype(jnp.bfloat16)
    blocks = seqs * length // BLK
    value_blocks = normed.reshape(blocks, BLK, HEADS, HEAD_DIM)
    id_blocks = segments.reshape(blocks, BLK)
    mixing_f = mixing.astype(jnp.float32)
    bias_f = jnp.transpose(mixing_bias.astype(jnp.float32))[:, :, None]

    def one_block(pair_item):
        block_values, block_ids = pair_item
        same_doc = block_ids[:, None] == block_ids[None, :]
        masked = jnp.where(same_doc[None, :, :], mixing_f, jnp.zeros((), jnp.float32))
        summed = jnp.einsum('hts,shd->thd', masked, block_values.astype(jnp.float32))
        return (summed + bias_f).astype(jnp.bfloat16)
    mixed = lax.map(one_block, (value_blocks, id_blocks)).reshape(seqs, length, width)
    gate_f = jax.nn.gelu(gate_in.astype(jnp.float32))
    return (gate_f * mixed.astype(jnp.float32)).astype(jnp.bfloat16)
```

```python
import functools

import jax
import jax.numpy as jnp
from jax import lax
from jax.experimental import pallas as pl
from jax.experimental.pallas import tpu as pltpu
from jax.sharding import PartitionSpec as P

HEAD_DIM = 128
LANES = 128
ID_ROWS = 16

epsilon = 1e-06


def pack_kernel(seg_ref, value_ref, out_ref):
    tokens = value_ref.shape[0]
    act = jax.nn.gelu(value_ref[...].astype(jnp.float32))
    scaled = act * lax.rsqrt(jnp.mean(act * act, axis=-1, keepdims=True) + epsilon)
    out_ref[0, :tokens, :] = scaled.astype(jnp.bfloat16)
    ids = seg_ref[...].astype(jnp.float32)
    rows = [ids[:, i * LANES:(i + 1) * LANES] for i in range(tokens // LANES)]
    rows.append(jnp.zeros((ID_ROWS - len(rows), LANES), jnp.float32))
    out_ref[0, tokens:, :] = jnp.concatenate(rows, axis=0).astype(jnp.bfloat16)


def pack(segments, values):
    tokens, width = values.shape
    heads = width // HEAD_DIM
    return pl.pallas_call(
        pack_kernel,
        grid=(heads,),
        in_specs=[
            pl.BlockSpec((1, tokens), lambda h: (0, 0)),
            pl.BlockSpec((tokens, HEAD_DIM), lambda h: (0, h)),
        ],
        out_specs=pl.BlockSpec((1, tokens + ID_ROWS, HEAD_DIM), lambda h: (h, 0, 0)),
        out_shape=jax.ShapeDtypeStruct((heads, tokens + ID_ROWS, HEAD_DIM), jnp.bfloat16),
        name="pack",
    )(segments, values)


def column(row):
    return jnp.broadcast_to(row, (LANES, LANES)).T


def mix_kernel(pos_ref, recv_ref, gain_ref, bias_ref, *rest, tokens, count):
    pieces, (out_ref, m_ref, ids_ref, biasc_ref, v_ref, sems) = rest[:count], rest[count:]
    blocks, block_len, _ = out_ref.shape
    shards = block_len // tokens
    rows = block_len // count

    def copy(i):
        start = pl.multiple_of(pos_ref[i] * rows, rows)
        return pltpu.make_async_copy(pieces[i].at[0], m_ref.at[pl.ds(start, rows)], sems.at[i])

    for i in range(count):
        copy(i).start()
    gain = gain_ref[...].astype(jnp.float32)
    for c in range(block_len // LANES):
        biasc_ref[c * LANES:(c + 1) * LANES, :] = column(
            bias_ref[:, c * LANES:(c + 1) * LANES].astype(jnp.float32)
        )
    for i in range(count):
        copy(i).wait()

    for q in range(blocks):
        lows, highs = [], []
        for j in range(shards):
            tile = recv_ref[q * shards + j, tokens:, :].astype(jnp.float32)
            used = tile[:tokens // LANES]
            lows.append(jnp.min(used))
            highs.append(jnp.max(used))
            for i in range(tokens // LANES):
                base = j * tokens + i * LANES
                ids_ref[base:base + LANES, :] = column(tile[i:i + 1])
        low = functools.reduce(jnp.minimum, lows).astype(jnp.int32)
        high = functools.reduce(jnp.maximum, highs).astype(jnp.int32)

        def part(doc):
            here = ids_ref[...] == doc.astype(jnp.float32)
            for j in range(shards):
                at = slice(j * tokens, (j + 1) * tokens)
                values = recv_ref[q * shards + j, :tokens, :].astype(jnp.float32)
                v_ref[at, :] = jnp.where(here[at], values, 0.0).astype(jnp.bfloat16)
            summed = jnp.dot(m_ref[...], v_ref[...], preferred_element_type=jnp.float32)
            return here, summed * gain + biasc_ref[...]

        out_ref[q] = part(low)[1].astype(jnp.bfloat16)

        def more(doc, _):
            here, result = part(doc)
            old = out_ref[q].astype(jnp.float32)
            out_ref[q] = jnp.where(here, result, old).astype(jnp.bfloat16)
            return 0

        lax.fori_loop(low + 1, high + 1, more, 0)


def mix(positions, recv, gain, bias, pieces, tokens):
    count = len(pieces)
    block_len = pieces[0].shape[2]
    blocks = recv.shape[0] * tokens // block_len
    vmem = pl.BlockSpec(memory_space=pltpu.VMEM)
    return pl.pallas_call(
        functools.partial(mix_kernel, tokens=tokens, count=count),
        in_specs=[pl.BlockSpec(memory_space=pltpu.SMEM), vmem, vmem, vmem]
        + [pl.BlockSpec(memory_space=pl.ANY)] * count,
        out_specs=vmem,
        out_shape=jax.ShapeDtypeStruct((blocks, block_len, HEAD_DIM), jnp.bfloat16),
        scratch_shapes=[
            pltpu.VMEM((block_len, block_len), jnp.bfloat16),
            pltpu.VMEM((block_len, HEAD_DIM), jnp.float32),
            pltpu.VMEM((block_len, HEAD_DIM), jnp.float32),
            pltpu.VMEM((block_len, HEAD_DIM), jnp.bfloat16),
            pltpu.SemaphoreType.DMA((count,)),
        ],
        name="mix",
    )(positions, recv, gain, bias, *pieces)


def gate_kernel(gate_ref, mixed_ref, out_ref):
    gate = jax.nn.gelu(gate_ref[...].astype(jnp.float32))
    out_ref[...] = (gate * mixed_ref[0].astype(jnp.float32)).astype(jnp.bfloat16)


def apply_gate(gate_in, mixed):
    heads, tokens, head_dim = mixed.shape
    spec = pl.BlockSpec((tokens, head_dim), lambda h: (0, h))
    return pl.pallas_call(
        gate_kernel,
        grid=(heads,),
        in_specs=[spec, pl.BlockSpec((1, tokens, head_dim), lambda h: (h, 0, 0))],
        out_specs=spec,
        out_shape=jax.ShapeDtypeStruct(gate_in.shape, jnp.bfloat16),
        name="gate",
    )(gate_in, mixed)


def gather_rows(mixing):
    n = lax.axis_size("dp")
    me = lax.axis_index("dp")
    pieces, places = [], []
    for step in range(0, n, 2):
        piece = mixing
        if step:
            piece = lax.ppermute(mixing, "dp", [(i, (i + step) % n) for i in range(n)])
        other = lax.ppermute(piece, "dp", [(i, i ^ 1) for i in range(n)])
        place = (me + n - step) % n
        pieces += [piece, other]
        places += [place, place ^ 1]
    return pieces, jnp.stack(places).astype(jnp.int32)


def per_device(gate_in, value_in, segments, value_gain, mixing, mixing_bias):
    tokens = value_in.shape[1]
    pieces, places = gather_rows(mixing)
    packed = pack(segments, value_in[0])
    recv = lax.all_to_all(packed, "sp", split_axis=0, concat_axis=0, tiled=True)
    mixed = mix(places, recv, value_gain[None, :], mixing_bias, pieces, tokens)
    mixed = mixed.reshape(-1, tokens, HEAD_DIM)
    returned = lax.all_to_all(mixed, "sp", split_axis=0, concat_axis=0, tiled=True)
    return apply_gate(gate_in[0], returned)[None]


def solution(mesh):
    return jax.shard_map(
        per_device,
        mesh=mesh,
        in_specs=(
            P("dp", "sp", None),
            P("dp", "sp", None),
            P("dp", "sp"),
            P("sp"),
            P("sp", "dp", None),
            P("sp", None),
        ),
        out_specs=P("dp", "sp", None),
        check_vma=False,
    )
```

```python
import functools

import jax
import jax.numpy as jnp
from jax import lax
from jax.experimental import pallas as pl
from jax.experimental.pallas import tpu as pltpu
from jax.sharding import PartitionSpec as P

HEAD_DIM = 128
LANES = 128
ID_ROWS = 16

epsilon = 1e-06


def pack_kernel(me_ref, seg_ref, *refs):
    half = len(refs) // 2
    tokens = refs[0].shape[0]
    ids = seg_ref[...].astype(jnp.float32)
    rows = [ids[:, i * LANES:(i + 1) * LANES] for i in range(tokens // LANES)]
    rows.append(jnp.zeros((ID_ROWS - len(rows), LANES), jnp.float32))
    tail = jnp.concatenate(rows, axis=0).astype(jnp.bfloat16)
    for value_ref, out_ref in zip(refs[:half], refs[half:]):
        out_ref[:tokens, :] = value_ref[...]
        out_ref[tokens:, :] = tail


def pack(me, segments, values):
    tokens, width = values.shape
    peers = width // HEAD_DIM
    return pl.pallas_call(
        pack_kernel,
        grid_spec=pltpu.PrefetchScalarGridSpec(
            num_scalar_prefetch=1,
            grid=(1,),
            in_specs=[pl.BlockSpec((1, tokens), lambda g, m: (0, 0))]
            + [
                pl.BlockSpec((tokens, HEAD_DIM), lambda g, m, k=k: (0, m[0] ^ k))
                for k in range(peers)
            ],
            out_specs=[pl.BlockSpec((tokens + ID_ROWS, HEAD_DIM), lambda g, m: (0, 0))] * peers,
        ),
        out_shape=[jax.ShapeDtypeStruct((tokens + ID_ROWS, HEAD_DIM), jnp.bfloat16)] * peers,
        name="pack",
    )(me, segments, *[values] * peers)


def assemble_kernel(pos_ref, *rest):
    count = len(rest) - 2
    pieces, out_ref, sems = rest[:count], rest[count], rest[count + 1]
    rows = out_ref.shape[0] // count

    def copy(i):
        start = pl.multiple_of(pos_ref[i] * rows, rows)
        return pltpu.make_async_copy(pieces[i].at[0], out_ref.at[pl.ds(start, rows)], sems.at[i])

    for i in range(count):
        copy(i).start()
    for i in range(count):
        copy(i).wait()


def assemble(places, pieces):
    count, length = len(pieces), pieces[0].shape[2]
    return pl.pallas_call(
        assemble_kernel,
        in_specs=[pl.BlockSpec(memory_space=pltpu.SMEM)]
        + [pl.BlockSpec(memory_space=pltpu.VMEM)] * count,
        out_specs=pl.BlockSpec(memory_space=pltpu.VMEM),
        out_shape=jax.ShapeDtypeStruct((length, length), jnp.bfloat16),
        scratch_shapes=[pltpu.SemaphoreType.DMA((count,))],
        name="assemble",
    )(places, *pieces)


def column(row):
    return jnp.broadcast_to(row, (LANES, LANES)).T


def mix_kernel(me_ref, m_ref, gain_ref, bias_ref, *rest, shards):
    recvs, outs = rest[:shards], rest[shards:2 * shards]
    ids_ref, values_ref, part_ref, mixed_ref = rest[2 * shards:]
    tokens = outs[0].shape[0]
    block_len = m_ref.shape[0]
    gain = gain_ref[...].astype(jnp.float32)
    bias = bias_ref[...].astype(jnp.float32)
    lows, highs, starts = [], [], []
    for j in range(shards):
        start = pl.multiple_of(((me_ref[0] ^ j) & (shards - 1)) * tokens, tokens)
        starts.append(start)
        tile = recvs[j][tokens:, :].astype(jnp.float32)
        used = tile[:tokens // LANES]
        lows.append(jnp.min(used))
        highs.append(jnp.max(used))
        for i in range(tokens // LANES):
            ids_ref[pl.ds(start + i * LANES, LANES), :] = column(tile[i:i + 1])
        act = jax.nn.gelu(recvs[j][:tokens, :].astype(jnp.float32))
        scaled = act * lax.rsqrt(jnp.mean(act * act, axis=-1, keepdims=True) + epsilon)
        values_ref[pl.ds(start, tokens), :] = (scaled * gain).astype(jnp.bfloat16)
    low = functools.reduce(jnp.minimum, lows).astype(jnp.int32)
    high = functools.reduce(jnp.maximum, highs).astype(jnp.int32)
    biasc = jnp.concatenate(
        [column(bias[:, c * LANES:(c + 1) * LANES]) for c in range(block_len // LANES)], axis=0
    )

    def part(doc):
        here = ids_ref[...] == doc.astype(jnp.float32)
        values = values_ref[...].astype(jnp.float32)
        part_ref[...] = jnp.where(here, values, 0.0).astype(jnp.bfloat16)
        return here, jnp.dot(m_ref[...], part_ref[...], preferred_element_type=jnp.float32)

    mixed_ref[...] = part(low)[1] + biasc

    def more(doc, _):
        here, result = part(doc)
        mixed_ref[...] = jnp.where(here, result + biasc, mixed_ref[...])
        return 0

    lax.fori_loop(low + 1, high + 1, more, 0)
    for j in range(shards):
        outs[j][...] = mixed_ref[pl.ds(starts[j], tokens), :].astype(jnp.bfloat16)


def mix(me, matrix, gain, bias, recvs):
    shards = len(recvs)
    block_len = matrix.shape[0]
    tokens = block_len // shards
    vmem = pl.BlockSpec(memory_space=pltpu.VMEM)
    return pl.pallas_call(
        functools.partial(mix_kernel, shards=shards),
        in_specs=[pl.BlockSpec(memory_space=pltpu.SMEM)] + [vmem] * (3 + shards),
        out_specs=[vmem] * shards,
        out_shape=[jax.ShapeDtypeStruct((tokens, HEAD_DIM), jnp.bfloat16)] * shards,
        scratch_shapes=[
            pltpu.VMEM((block_len, HEAD_DIM), jnp.float32),
            pltpu.VMEM((block_len, HEAD_DIM), jnp.bfloat16),
            pltpu.VMEM((block_len, HEAD_DIM), jnp.bfloat16),
            pltpu.VMEM((block_len, HEAD_DIM), jnp.float32),
        ],
        name="mix",
    )(me, matrix, gain, bias, *recvs)


def gate_kernel(me_ref, gate_ref, *rest, shards):
    mixeds, out_ref = rest[:shards], rest[-1]
    gate = jax.nn.gelu(gate_ref[...].astype(jnp.float32))
    for j in range(shards):
        @pl.when(pl.program_id(0) == j)
        def _():
            out_ref[...] = (gate * mixeds[j][...].astype(jnp.float32)).astype(jnp.bfloat16)


def apply_gate(me, base, gate_in, mixeds, before):
    shards = len(mixeds)
    tokens, head_dim = mixeds[0].shape
    spec = pl.BlockSpec((tokens, head_dim), lambda j, m: (0, m[0] ^ base ^ j))
    whole = pl.BlockSpec((tokens, head_dim), lambda j, m: (0, 0))
    extra = [] if before is None else [before]
    return pl.pallas_call(
        functools.partial(gate_kernel, shards=shards),
        grid_spec=pltpu.PrefetchScalarGridSpec(
            num_scalar_prefetch=1,
            grid=(shards,),
            in_specs=[spec] + [whole] * shards + [pl.BlockSpec(memory_space=pl.ANY)] * len(extra),
            out_specs=spec,
        ),
        out_shape=jax.ShapeDtypeStruct(gate_in.shape, jnp.bfloat16),
        input_output_aliases={2 + shards: 0} if extra else {},
        name="gate",
    )(me, gate_in, *mixeds, *extra)


def gather_rows(mixing):
    n = lax.axis_size("dp")
    me = lax.axis_index("dp")
    pieces, places = [], []
    for step in range(0, n, 2):
        piece = mixing
        if step:
            piece = lax.ppermute(mixing, "dp", [(i, (i + step) % n) for i in range(n)])
        other = lax.ppermute(piece, "dp", [(i, i ^ 1) for i in range(n)])
        place = (me + n - step) % n
        pieces += [piece, other]
        places += [place, place ^ 1]
    return pieces, jnp.stack(places).astype(jnp.int32)


def per_device(gate_in, value_in, segments, value_gain, mixing, mixing_bias):
    peers = lax.axis_size("sp")
    tokens = value_in.shape[1]
    shards = mixing.shape[2] // tokens
    me = lax.axis_index("sp").astype(jnp.int32)[None]

    def swap(array, k):
        if k == 0:
            return array
        return lax.ppermute(array, "sp", [(i, i ^ k) for i in range(peers)])

    packed, mixing = lax.optimization_barrier((pack(me, segments, value_in[0]), mixing))
    groups = [[base + j for j in range(shards)] for base in range(0, peers, shards)]
    recvs = [[swap(packed[k], k) for k in ks] for ks in groups]
    pieces, places = gather_rows(mixing)
    matrix = assemble(places, pieces)
    gain = value_gain[None, :]
    mixed = [mix(me, matrix, gain, mixing_bias, group) for group in recvs]
    returned = [[swap(a, k) for a, k in zip(m, ks)] for m, ks in zip(mixed, groups)]
    out = None
    for ks, group in zip(groups, returned):
        out = apply_gate(me, ks[0], gate_in[0], group, out)
    return out[None]


def solution(mesh):
    return jax.shard_map(
        per_device,
        mesh=mesh,
        in_specs=(
            P("dp", "sp", None),
            P("dp", "sp", None),
            P("dp", "sp"),
            P("sp"),
            P("sp", "dp", None),
            P("sp", None),
        ),
        out_specs=P("dp", "sp", None),
        check_vma=False,
    )
```

```python
import functools

import jax
import jax.numpy as jnp
from jax import lax
from jax.experimental import pallas as pl
from jax.experimental.pallas import tpu as pltpu
from jax.sharding import PartitionSpec as P

HEAD_DIM = 128
LANES = 128
ID_ROWS = 16
NEAR_BYTES = 2 << 20

epsilon = 1e-06


def pack_kernel(me_ref, seg_ref, *refs):
    half = len(refs) // 2
    tokens = refs[0].shape[0]
    ids = seg_ref[...].astype(jnp.float32)
    rows = [ids[:, i * LANES:(i + 1) * LANES] for i in range(tokens // LANES)]
    rows.append(jnp.zeros((ID_ROWS - len(rows), LANES), jnp.float32))
    tail = jnp.concatenate(rows, axis=0).astype(jnp.bfloat16)
    for value_ref, out_ref in zip(refs[:half], refs[half:]):
        out_ref[:tokens, :] = value_ref[...]
        out_ref[tokens:, :] = tail


def pack(me, segments, values):
    tokens, width = values.shape
    peers = width // HEAD_DIM
    return pl.pallas_call(
        pack_kernel,
        grid_spec=pltpu.PrefetchScalarGridSpec(
            num_scalar_prefetch=1,
            grid=(1,),
            in_specs=[pl.BlockSpec((1, tokens), lambda g, m: (0, 0))]
            + [
                pl.BlockSpec((tokens, HEAD_DIM), lambda g, m, k=k: (0, m[0] ^ k))
                for k in range(peers)
            ],
            out_specs=[pl.BlockSpec((tokens + ID_ROWS, HEAD_DIM), lambda g, m: (0, 0))] * peers,
        ),
        out_shape=[jax.ShapeDtypeStruct((tokens + ID_ROWS, HEAD_DIM), jnp.bfloat16)] * peers,
        name="pack",
    )(me, segments, *[values] * peers)


def assemble_kernel(pos_ref, *rest):
    count = len(rest) - 2
    pieces, out_ref, sems = rest[:count], rest[count], rest[count + 1]
    rows = out_ref.shape[0] // count

    def copy(i):
        start = pl.multiple_of(pos_ref[i] * rows, rows)
        return pltpu.make_async_copy(pieces[i].at[0], out_ref.at[pl.ds(start, rows)], sems.at[i])

    for i in range(count):
        copy(i).start()
    for i in range(count):
        copy(i).wait()


def assemble(places, pieces):
    count, length = len(pieces), pieces[0].shape[2]
    return pl.pallas_call(
        assemble_kernel,
        in_specs=[pl.BlockSpec(memory_space=pltpu.SMEM)]
        + [pl.BlockSpec(memory_space=pltpu.VMEM)] * count,
        out_specs=pl.BlockSpec(memory_space=pltpu.VMEM),
        out_shape=jax.ShapeDtypeStruct((length, length), jnp.bfloat16),
        scratch_shapes=[pltpu.SemaphoreType.DMA((count,))],
        name="assemble",
    )(places, *pieces)


def column(row):
    return jnp.broadcast_to(row, (LANES, LANES)).T


def mix_kernel(me_ref, m_ref, gain_ref, bias_ref, *rest, shards):
    recvs, outs = rest[:shards], rest[shards:2 * shards]
    ids_ref, values_ref, part_ref, mixed_ref = rest[2 * shards:]
    tokens = outs[0].shape[0]
    block_len = m_ref.shape[0]
    gain = gain_ref[...].astype(jnp.float32)
    bias = bias_ref[...].astype(jnp.float32)
    lows, highs, starts = [], [], []
    for j in range(shards):
        start = pl.multiple_of(((me_ref[0] ^ j) & (shards - 1)) * tokens, tokens)
        starts.append(start)
        tile = recvs[j][tokens:, :].astype(jnp.float32)
        used = tile[:tokens // LANES]
        lows.append(jnp.min(used))
        highs.append(jnp.max(used))
        for i in range(tokens // LANES):
            ids_ref[pl.ds(start + i * LANES, LANES), :] = column(tile[i:i + 1])
        act = jax.nn.gelu(recvs[j][:tokens, :].astype(jnp.float32))
        scaled = act * lax.rsqrt(jnp.mean(act * act, axis=-1, keepdims=True) + epsilon)
        values_ref[pl.ds(start, tokens), :] = (scaled * gain).astype(jnp.bfloat16)
    low = functools.reduce(jnp.minimum, lows).astype(jnp.int32)
    high = functools.reduce(jnp.maximum, highs).astype(jnp.int32)
    biasc = jnp.concatenate(
        [column(bias[:, c * LANES:(c + 1) * LANES]) for c in range(block_len // LANES)], axis=0
    )

    def part(doc):
        here = ids_ref[...] == doc.astype(jnp.float32)
        values = values_ref[...].astype(jnp.float32)
        part_ref[...] = jnp.where(here, values, 0.0).astype(jnp.bfloat16)
        return here, jnp.dot(m_ref[...], part_ref[...], preferred_element_type=jnp.float32)

    mixed_ref[...] = part(low)[1] + biasc

    def more(doc, _):
        here, result = part(doc)
        mixed_ref[...] = jnp.where(here, result + biasc, mixed_ref[...])
        return 0

    lax.fori_loop(low + 1, high + 1, more, 0)
    for j in range(shards):
        outs[j][...] = mixed_ref[pl.ds(starts[j], tokens), :].astype(jnp.bfloat16)


def mix(me, matrix, gain, bias, recvs):
    shards = len(recvs)
    block_len = matrix.shape[0]
    tokens = block_len // shards
    vmem = pl.BlockSpec(memory_space=pltpu.VMEM)
    return pl.pallas_call(
        functools.partial(mix_kernel, shards=shards),
        in_specs=[pl.BlockSpec(memory_space=pltpu.SMEM)] + [vmem] * (3 + shards),
        out_specs=[vmem] * shards,
        out_shape=[jax.ShapeDtypeStruct((tokens, HEAD_DIM), jnp.bfloat16)] * shards,
        scratch_shapes=[
            pltpu.VMEM((block_len, HEAD_DIM), jnp.float32),
            pltpu.VMEM((block_len, HEAD_DIM), jnp.bfloat16),
            pltpu.VMEM((block_len, HEAD_DIM), jnp.bfloat16),
            pltpu.VMEM((block_len, HEAD_DIM), jnp.float32),
        ],
        name="mix",
    )(me, matrix, gain, bias, *recvs)


def gate_kernel(me_ref, gate_ref, *rest, shards):
    mixeds, out_ref = rest[:shards], rest[-1]
    gate = jax.nn.gelu(gate_ref[...].astype(jnp.float32))
    for j in range(shards):
        @pl.when(pl.program_id(0) == j)
        def _():
            out_ref[...] = (gate * mixeds[j][...].astype(jnp.float32)).astype(jnp.bfloat16)


def apply_gate(me, base, gate_in, mixeds, before):
    shards = len(mixeds)
    tokens, head_dim = mixeds[0].shape
    spec = pl.BlockSpec((tokens, head_dim), lambda j, m: (0, m[0] ^ (base + j)))
    whole = pl.BlockSpec(memory_space=pltpu.VMEM)
    extra = [] if before is None else [before]
    return pl.pallas_call(
        functools.partial(gate_kernel, shards=shards),
        grid_spec=pltpu.PrefetchScalarGridSpec(
            num_scalar_prefetch=1,
            grid=(shards,),
            in_specs=[spec] + [whole] * shards + [pl.BlockSpec(memory_space=pl.ANY)] * len(extra),
            out_specs=spec,
        ),
        out_shape=jax.ShapeDtypeStruct(gate_in.shape, jnp.bfloat16),
        input_output_aliases={2 + shards: 0} if extra else {},
        name="gate",
    )(me, gate_in, *mixeds, *extra)


def near(array, copies):
    if copies * array.size * array.dtype.itemsize > NEAR_BYTES:
        return array
    return pltpu.with_memory_space_constraint(array, pltpu.VMEM)


def gather_rows(mixing, first):
    n = lax.axis_size("dp")
    me = lax.axis_index("dp")
    pieces, places = [], []
    for step in range(0, n, 2):
        piece = mixing
        if step:
            piece = lax.ppermute(mixing, "dp", [(i, (i + step) % n) for i in range(n)])
            piece = lax.optimization_barrier((piece, first))[0]
        other = lax.ppermute(piece, "dp", [(i, i ^ 1) for i in range(n)])
        place = (me + n - step) % n
        pieces += [piece, other]
        places += [place, place ^ 1]
    return pieces, jnp.stack(places).astype(jnp.int32)


def per_device(gate_in, value_in, segments, value_gain, mixing, mixing_bias):
    peers = lax.axis_size("sp")
    tokens = value_in.shape[1]
    shards = mixing.shape[2] // tokens
    me = lax.axis_index("sp").astype(jnp.int32)[None]

    def swap(array, k):
        if k == 0:
            return array
        return near(lax.ppermute(array, "sp", [(i, i ^ k) for i in range(peers)]), peers)

    packed, mixing = lax.optimization_barrier((pack(me, segments, value_in[0]), mixing))
    groups = [[base + j for j in range(shards)] for base in range(0, peers, shards)]
    recvs = [[swap(packed[k], k) for k in ks] for ks in groups]
    pieces, places = gather_rows(mixing, [a for group in recvs for a in group][1:])
    matrix = assemble(places, pieces)
    gain = value_gain[None, :]
    mixed = [mix(me, matrix, gain, mixing_bias, group) for group in recvs]
    returned = [[swap(a, k) for a, k in zip(m, ks)] for m, ks in zip(mixed, groups)]
    early = [a for group in returned[:-1] for a in group]
    out = apply_gate(me, 0, gate_in[0], early, None)
    out = apply_gate(me, len(early), gate_in[0], returned[-1], out)
    return out[None]


def solution(mesh):
    return jax.shard_map(
        per_device,
        mesh=mesh,
        in_specs=(
            P("dp", "sp", None),
            P("dp", "sp", None),
            P("dp", "sp"),
            P("sp"),
            P("sp", "dp", None),
            P("sp", None),
        ),
        out_specs=P("dp", "sp", None),
        check_vma=False,
    )
```

```python
import functools

import jax
import jax.numpy as jnp
from jax import lax
from jax.experimental import pallas as pl
from jax.experimental.pallas import tpu as pltpu
from jax.sharding import PartitionSpec as P

HEAD_DIM = 128
LANES = 128
ID_ROWS = 16
NEAR_BYTES = 2 << 20

epsilon = 1e-06


def pack_kernel(me_ref, seg_ref, *refs):
    half = len(refs) // 2
    tokens = refs[0].shape[0]
    ids = seg_ref[...].astype(jnp.float32)
    rows = [ids[:, i * LANES:(i + 1) * LANES] for i in range(tokens // LANES)]
    rows.append(jnp.zeros((ID_ROWS - len(rows), LANES), jnp.float32))
    tail = jnp.concatenate(rows, axis=0).astype(jnp.bfloat16)
    for value_ref, out_ref in zip(refs[:half], refs[half:]):
        out_ref[:tokens, :] = value_ref[...]
        out_ref[tokens:, :] = tail


def pack(me, segments, values):
    tokens, width = values.shape
    peers = width // HEAD_DIM
    return pl.pallas_call(
        pack_kernel,
        grid_spec=pltpu.PrefetchScalarGridSpec(
            num_scalar_prefetch=1,
            grid=(1,),
            in_specs=[pl.BlockSpec((1, tokens), lambda g, m: (0, 0))]
            + [
                pl.BlockSpec((tokens, HEAD_DIM), lambda g, m, k=k: (0, m[0] ^ k))
                for k in range(peers)
            ],
            out_specs=[pl.BlockSpec((tokens + ID_ROWS, HEAD_DIM), lambda g, m: (0, 0))] * peers,
        ),
        out_shape=[jax.ShapeDtypeStruct((tokens + ID_ROWS, HEAD_DIM), jnp.bfloat16)] * peers,
        name="pack",
    )(me, segments, *[values] * peers)


def assemble_kernel(pos_ref, *rest):
    count = len(rest) - 2
    pieces, out_ref, sems = rest[:count], rest[count], rest[count + 1]
    rows = out_ref.shape[0] // count

    def copy(i):
        start = pl.multiple_of(pos_ref[i] * rows, rows)
        return pltpu.make_async_copy(pieces[i].at[0], out_ref.at[pl.ds(start, rows)], sems.at[i])

    for i in range(count):
        copy(i).start()
    for i in range(count):
        copy(i).wait()


def assemble(places, pieces):
    count, length = len(pieces), pieces[0].shape[2]
    return pl.pallas_call(
        assemble_kernel,
        in_specs=[pl.BlockSpec(memory_space=pltpu.SMEM)]
        + [pl.BlockSpec(memory_space=pl.ANY)] * count,
        out_specs=pl.BlockSpec(memory_space=pltpu.VMEM),
        out_shape=jax.ShapeDtypeStruct((length, length), jnp.bfloat16),
        scratch_shapes=[pltpu.SemaphoreType.DMA((count,))],
        name="assemble",
    )(places, *pieces)


def column(row):
    return jnp.broadcast_to(row, (LANES, LANES)).T


def mix_kernel(me_ref, m_ref, gain_ref, bias_ref, *rest, shards):
    recvs, outs = rest[:shards], rest[shards:2 * shards]
    ids_ref, values_ref, part_ref, mixed_ref = rest[2 * shards:]
    tokens = outs[0].shape[0]
    block_len = m_ref.shape[0]
    gain = gain_ref[...].astype(jnp.float32)
    bias = bias_ref[...].astype(jnp.float32)
    lows, highs, starts = [], [], []
    for j in range(shards):
        start = pl.multiple_of(((me_ref[0] ^ j) & (shards - 1)) * tokens, tokens)
        starts.append(start)
        tile = recvs[j][tokens:, :].astype(jnp.float32)
        used = tile[:tokens // LANES]
        lows.append(jnp.min(used))
        highs.append(jnp.max(used))
        for i in range(tokens // LANES):
            ids_ref[pl.ds(start + i * LANES, LANES), :] = column(tile[i:i + 1])
        act = jax.nn.gelu(recvs[j][:tokens, :].astype(jnp.float32))
        scaled = act * lax.rsqrt(jnp.mean(act * act, axis=-1, keepdims=True) + epsilon)
        values_ref[pl.ds(start, tokens), :] = (scaled * gain).astype(jnp.bfloat16)
    low = functools.reduce(jnp.minimum, lows).astype(jnp.int32)
    high = functools.reduce(jnp.maximum, highs).astype(jnp.int32)
    biasc = jnp.concatenate(
        [column(bias[:, c * LANES:(c + 1) * LANES]) for c in range(block_len // LANES)], axis=0
    )

    def part(doc):
        here = ids_ref[...] == doc.astype(jnp.float32)
        values = values_ref[...].astype(jnp.float32)
        part_ref[...] = jnp.where(here, values, 0.0).astype(jnp.bfloat16)
        return here, jnp.dot(m_ref[...], part_ref[...], preferred_element_type=jnp.float32)

    mixed_ref[...] = part(low)[1] + biasc

    def more(doc, _):
        here, result = part(doc)
        mixed_ref[...] = jnp.where(here, result + biasc, mixed_ref[...])
        return 0

    lax.fori_loop(low + 1, high + 1, more, 0)
    for j in range(shards):
        outs[j][...] = mixed_ref[pl.ds(starts[j], tokens), :].astype(jnp.bfloat16)


def mix(me, matrix, gain, bias, recvs):
    shards = len(recvs)
    block_len = matrix.shape[0]
    tokens = block_len // shards
    vmem = pl.BlockSpec(memory_space=pltpu.VMEM)
    return pl.pallas_call(
        functools.partial(mix_kernel, shards=shards),
        in_specs=[pl.BlockSpec(memory_space=pltpu.SMEM)] + [vmem] * (3 + shards),
        out_specs=[vmem] * shards,
        out_shape=[jax.ShapeDtypeStruct((tokens, HEAD_DIM), jnp.bfloat16)] * shards,
        scratch_shapes=[
            pltpu.VMEM((block_len, HEAD_DIM), jnp.float32),
            pltpu.VMEM((block_len, HEAD_DIM), jnp.bfloat16),
            pltpu.VMEM((block_len, HEAD_DIM), jnp.bfloat16),
            pltpu.VMEM((block_len, HEAD_DIM), jnp.float32),
        ],
        name="mix",
    )(me, matrix, gain, bias, *recvs)


def gate_kernel(me_ref, gate_ref, *rest, shards):
    mixeds, out_ref = rest[:shards], rest[-1]
    gate = jax.nn.gelu(gate_ref[...].astype(jnp.float32))
    for j in range(shards):
        @pl.when(pl.program_id(0) == j)
        def _():
            out_ref[...] = (gate * mixeds[j][...].astype(jnp.float32)).astype(jnp.bfloat16)


def apply_gate(me, base, gate_in, mixeds, before):
    shards = len(mixeds)
    tokens, head_dim = mixeds[0].shape
    spec = pl.BlockSpec((tokens, head_dim), lambda j, m: (0, m[0] ^ (base + j)))
    whole = pl.BlockSpec(memory_space=pltpu.VMEM)
    extra = [] if before is None else [before]
    return pl.pallas_call(
        functools.partial(gate_kernel, shards=shards),
        grid_spec=pltpu.PrefetchScalarGridSpec(
            num_scalar_prefetch=1,
            grid=(shards,),
            in_specs=[spec] + [whole] * shards + [pl.BlockSpec(memory_space=pl.ANY)] * len(extra),
            out_specs=spec,
        ),
        out_shape=jax.ShapeDtypeStruct(gate_in.shape, jnp.bfloat16),
        input_output_aliases={2 + shards: 0} if extra else {},
        name="gate",
    )(me, gate_in, *mixeds, *extra)


def near(array, copies):
    if copies * array.size * array.dtype.itemsize > NEAR_BYTES:
        return array
    return pltpu.with_memory_space_constraint(array, pltpu.VMEM)


def gather_rows(mixing, first):
    n = lax.axis_size("dp")
    me = lax.axis_index("dp")
    pieces, places = [], []
    for step in range(0, n, 2):
        piece = mixing
        if step:
            piece = lax.ppermute(mixing, "dp", [(i, (i + step) % n) for i in range(n)])
            piece = lax.optimization_barrier((piece, first))[0]
        other = lax.ppermute(piece, "dp", [(i, i ^ 1) for i in range(n)])
        place = (me + n - step) % n
        pieces += [piece, other]
        places += [place, place ^ 1]
    return pieces, jnp.stack(places).astype(jnp.int32)


def per_device(gate_in, value_in, segments, value_gain, mixing, mixing_bias):
    peers = lax.axis_size("sp")
    tokens = value_in.shape[1]
    shards = mixing.shape[2] // tokens
    me = lax.axis_index("sp").astype(jnp.int32)[None]

    def swap(array, k):
        if k == 0:
            return array
        return near(lax.ppermute(array, "sp", [(i, i ^ k) for i in range(peers)]), peers)

    packed, mixing = lax.optimization_barrier((pack(me, segments, value_in[0]), mixing))
    groups = [[base + j for j in range(shards)] for base in range(0, peers, shards)]
    recvs = [[swap(packed[k], k) for k in ks] for ks in groups]
    pieces, places = gather_rows(mixing, [a for group in recvs for a in group][1:peers // 2 + 1])
    matrix = assemble(places, pieces)
    gain = value_gain[None, :]
    mixed = [mix(me, matrix, gain, mixing_bias, group) for group in recvs]
    returned = [[swap(a, k) for a, k in zip(m, ks)] for m, ks in zip(mixed, groups)]
    early = [a for group in returned[:-1] for a in group]
    out = apply_gate(me, 0, gate_in[0], early, None)
    out = apply_gate(me, len(early), gate_in[0], returned[-1], out)
    return out[None]


def solution(mesh):
    return jax.shard_map(
        per_device,
        mesh=mesh,
        in_specs=(
            P("dp", "sp", None),
            P("dp", "sp", None),
            P("dp", "sp"),
            P("sp"),
            P("sp", "dp", None),
            P("sp", None),
        ),
        out_specs=P("dp", "sp", None),
        check_vma=False,
    )
```
